32 devices in a mesh: grp: 2 (over x), ep: 16 (over z, y, core).
Axes of the slice: x: 2, y: 2, z: 4, core: 2. Of those that a mesh axis runs over, the one named last changes fastest.
Arguments:
- tokens: bfloat16 [1024, 2048], P(('grp', 'ep')), parts along dimension 0, may hold values from -6 to 6
- norm_gain: float32 [2048], replicated, may hold values from 0.5 to 4
- routes: int32 [1024, 4], P(('grp', 'ep')), parts along dimension 0, may hold values from 0 to 15, all different within a row; in each aligned block of 32 rows (0 to 31, 32 to 63, ...) at most 16 rows name the same one
- route_logits: float32 [1024, 4], P(('grp', 'ep')), parts along dimension 0, may hold values from -6 to 6
- w_gate: bfloat16 [16, 2048, 1792], P('ep'), may hold values from -0.125 to 0.125
- w_up: bfloat16 [16, 2048, 1792], P('ep'), may hold values from -0.125 to 0.125
- w_down: bfloat16 [16, 1792, 2048], P('ep'), may hold values from -0.125 to 0.125
Outputs:
- mixed: bfloat16 [1024, 2048], P(('grp', 'ep')), parts along dimension 0
The draws below stay inside these ranges and needn't reach their ends.
There are 2 independent parts, one for each index of `grp`. The reference program is written for one: setup_inputs(seed, part) draws one part's arguments, and reference() takes and returns one part's arrays. A program takes and returns all parts, laid end to end along the dimension named above; an argument that names none is the same for every part. Nothing has to cross between parts.
Inputs may be any that keep to these rules, and one draw needn't show every extreme that they name: `routes`: each token names 4 different experts. Among the 32 tokens of one device no expert is named by more than 16 of them, and in every draw some expert is named by exactly 16 tokens of some device.
All inputs are finite; a program needn't handle non-finite values.
Results may differ from the reference program's by a relative error of at most 0.012.
Values may be sent and summed in bfloat16 or wider, within the bound.
A program may use at most 64 MiB of HBM per device.

```python
import math
import jax
import jax.numpy as jnp
import numpy as np
from jax import lax

D = 2048
FF = 1792
TOP_K = 4
TOK_DEV = 32
EXPERTS = 16
CAP = 16
TOKENS = 512


def level_of(rng, extent, cuts, low, largest):
    level, own = 1.0, jax.random.fold_in(rng, 6)
    for dim, blocks in cuts:
        draws = jnp.exp(jax.random.uniform(jax.random.fold_in(own, dim), (blocks,), jnp.float32, low / len(cuts), largest / len(cuts)))
        level = level * jnp.repeat(draws, extent[dim] // blocks).reshape([-1 if axis == dim else 1 for axis in range(len(extent))])
    return level


def deal_out(own_key, own, number, rows, amount, top, reach, slope):
    sequence = jax.random.permutation(own_key, amount)
    packed, ordinary = load_shares(amount, rows * top, reach, slope, True), load_shares(amount, rows * top, reach, slope, False)
    places = jnp.arange(amount)

    def named(tallies, turn):
        used = int((tallies > 0).sum())
        fixed = max(1, used // 4)
        moved = fixed + (places - fixed + turn * (used - fixed)) % max(1, amount - fixed)
        return jnp.zeros((amount,), jnp.int32).at[sequence[jnp.where(places < fixed, places, moved)]].set(jnp.asarray(tallies, jnp.int32))

    tallies = jnp.where(number % 4 == 0, named(packed, number // 4), named(ordinary, number - number // 4 - 1))
    mixed = jax.random.permutation(jax.random.fold_in(own, 3), amount)
    giver, receiver = mixed[0:amount // 2 * 2:2], mixed[1:amount // 2 * 2:2]
    margin = jnp.minimum(tallies[giver] - 1, reach - tallies[receiver]) // 2
    margin = jnp.where((giver == sequence[0]) | (receiver == sequence[0]) | (tallies[receiver] == 0), 0, jnp.maximum(margin, 0))
    moved = jax.random.randint(jax.random.fold_in(own, 4), (amount // 2,), 0, 1 << 20) % (margin + 1)
    tallies = tallies.at[giver].add(-moved).at[receiver].add(moved)
    items = jnp.searchsorted(jnp.cumsum(tallies), jnp.arange(rows * top), side="right").astype(jnp.int32)
    grid = items.reshape(top, rows).T
    grid = grid[jax.random.permutation(jax.random.fold_in(own, 1), rows)]
    turn = jax.random.randint(jax.random.fold_in(own, 2), (rows, 1), 0, top)
    return jnp.take_along_axis(grid, (jnp.arange(top)[None, :] + turn) % top, axis=1)


def load_shares(count, total, bound, slope, full):
    portions = [(1 << 20) // math.isqrt(rank ** slope) + 1 for rank in range(1, count + 1)]
    largest = bound if full else min(bound, max(-(-total // count), total * portions[0] // sum(portions)))
    least = 1 if total - largest >= count - 1 else 0
    given, surplus = [largest] + [least] * (count - 1), total - largest - least * (count - 1)
    while surplus > 0:
        movable = [i for i in range(1, count) if given[i] < largest] or [i for i in range(1, count) if given[i] < bound]
        pool, left = sum([portions[i] for i in movable]), surplus
        for i in movable:
            addition = min(bound - given[i], max(1, left * portions[i] // pool), surplus)
            given[i] = given[i] + addition
            surplus = surplus - addition
    return np.array(given)


def centred(stream_key, shape, scale, limit, split=(), kind=jnp.bfloat16):
    factor_of = level_of(stream_key, shape, split, -0.22, 0.18) if split else 1.0
    drawn = jax.random.normal(stream_key, shape, jnp.float32) * scale * factor_of
    return jnp.minimum(jnp.maximum(drawn, -limit), limit).astype(kind)


def setup_inputs(seed: int = 0, part: int = 0) -> dict:
    arg_keys = jax.random.split(jax.random.key(seed), 8)
    part_keys = jax.random.split(jax.random.fold_in(arg_keys[7], part), 8)
    tokens = centred(part_keys[0], (TOKENS, D), 1.0, 6.0, ((0, 16),))
    norm_gain = jnp.clip(jnp.exp(jax.random.uniform(arg_keys[1], (D,), jnp.float32, math.log(0.5), math.log(4.0))), 0.5, 4.0)
    routes_keys = jax.random.split(jax.random.fold_in(part_keys[2], 1), TOKENS // TOK_DEV)
    routes_turns = jax.random.permutation(jax.random.fold_in(part_keys[2], 3), TOKENS // TOK_DEV)
    routes = jax.vmap(lambda own, number: deal_out(jax.random.fold_in(part_keys[2], 2), own, number, TOK_DEV, EXPERTS, TOP_K, CAP, 2))(routes_keys, routes_turns).reshape((TOKENS, TOP_K))
    route_logits = centred(part_keys[3], (TOKENS, TOP_K), 1.5, 6.0, ((0, 16),), jnp.float32)
    w_gate = centred(arg_keys[4], (EXPERTS, D, FF), D ** -0.5, 0.125, ((0, 16),))
    w_up = centred(arg_keys[5], (EXPERTS, D, FF), D ** -0.5, 0.125, ((0, 16),))
    w_down = centred(arg_keys[6], (EXPERTS, FF, D), FF ** -0.5, 0.125, ((0, 16),))
    return dict(tokens=tokens, norm_gain=norm_gain, routes=routes, route_logits=route_logits, w_gate=w_gate, w_up=w_up, w_down=w_down)


def rmsnorm(values, gain):
    floats = values.astype(jnp.float32)
    scaled = floats * lax.rsqrt(lax.optimization_barrier(jnp.mean(floats * floats, axis=-1, keepdims=True)) + 1e-06)
    return (scaled * gain.astype(jnp.float32)).astype(jnp.bfloat16)

def expert(rows, gate_weight, up_weight, down_weight):
    gate = jnp.minimum(jnp.dot(rows, gate_weight, preferred_element_type=jnp.float32), 7.0)
    upper = jnp.clip(jnp.dot(rows, up_weight, preferred_element_type=jnp.float32), -7.0, 7.0)
    active = (gate * jax.nn.sigmoid(1.702 * gate) * (upper + 1.0)).astype(jnp.bfloat16)
    return jnp.dot(active, down_weight, preferred_element_type=jnp.float32).astype(jnp.bfloat16)

def reference(tokens, norm_gain, routes, route_logits, w_gate, w_up, w_down):
    normed = rmsnorm(tokens, norm_gain)
    route_weights = jax.nn.softmax(route_logits.astype(jnp.float32), axis=-1)

    def add_expert(total, expert_id):
        weight = lax.optimization_barrier(jnp.sum(jnp.where(routes == expert_id, route_weights, 0.0), axis=1))
        output = expert(normed, w_gate[expert_id], w_up[expert_id], w_down[expert_id])
        return (total + weight[:, None] * output.astype(jnp.float32), None)
    start = jnp.zeros((tokens.shape[0], tokens.shape[1]), jnp.float32)
    total, _ = lax.scan(add_expert, start, jnp.arange(EXPERTS, dtype=jnp.int32))
    return total.astype(jnp.bfloat16)
```

```python
import functools

import jax
import jax.numpy as jnp
from jax import lax
from jax.experimental import pallas as pl
from jax.experimental.pallas import tpu as pltpu
from jax.sharding import PartitionSpec as P

TOP_K = 4
LANES = 128
TILE = 256
F32 = jnp.float32
BF16 = jnp.bfloat16


def flip(value, bits):
    out, bit = value, 1
    while bit <= bits:
        if bits & bit:
            out = out + bit - 2 * bit * ((value // bit) % 2)
        bit *= 2
    return out


def layer(n, cap, zs, ys, x_ref, gain_ref, meta_ref, wg_hbm, wu_hbm, wd_hbm, o_ref,
          wg, wu, wd, G, M, X, H, O, Psib, Pown, R1, Q, R2, T, R3, F4, R4,
          w_sem, m_send, m_recv, z_send, y_send, s_send, g_recv,
          r1_send, r1_recv, q_send, r2_recv, t_send, r3_recv, r4_send, r4_recv):
    me = lax.axis_index("ep")
    core = me % 2
    chip = me // 2
    z = chip // ys
    y = chip % ys
    sib = chip * 2 + 1 - core
    rows, width = x_ref.shape
    ff = wg.shape[1]
    half = width // 2
    chips = n // 2

    def dev(zz, yy, cc):
        return (zz * ys + yy) * 2 + cc

    def remote(src, dst, send, recv, target):
        return pltpu.make_async_remote_copy(
            src_ref=src, dst_ref=dst, send_sem=send, recv_sem=recv,
            device_id={"ep": target}, device_id_type=pl.DeviceIdType.MESH)

    loads = []
    for i, (src, dst) in enumerate(((wg_hbm, wg), (wu_hbm, wu), (wd_hbm, wd))):
        k = src.shape[1] // 2
        for h in range(2):
            c = pltpu.make_async_copy(src.at[0, pl.ds(h * k, k)], dst.at[pl.ds(h * k, k)], w_sem.at[i, h])
            c.start()
            loads.append(c)

    x = x_ref[...].astype(F32)
    normed = x * lax.rsqrt(jnp.mean(x * x, axis=-1, keepdims=True) + 1e-06) * gain_ref[...]
    G[me] = normed.astype(BF16)
    M[me] = meta_ref[...]

    barrier = pltpu.get_barrier_semaphore()
    for d in range(1, n):
        pl.semaphore_signal(barrier, inc=1, device_id={"ep": (me + d) % n},
                            device_id_type=pl.DeviceIdType.MESH)
    pl.semaphore_wait(barrier, n - 1)

    sends = []

    def go(copy):
        copy.start()
        sends.append(copy)

    def pass_on(src, send, target):
        go(remote(G.at[src], G.at[src], send, g_recv.at[src], target))

    def landed(src):
        remote(G.at[src], G.at[src], z_send.at[0], g_recv.at[src], sib).wait_recv()

    for d in range(1, n):
        go(remote(meta_ref, M.at[me], m_send.at[d], m_recv.at[me], (me + d) % n))
    for d in range(1, zs):
        pass_on(me, z_send.at[d], dev(flip(z, d), y, core))
    if ys > 1:
        pass_on(me, y_send.at[0], dev(z, 1 - y, core))
    pass_on(me, s_send.at[0], sib)
    for d in range(1, zs):
        src = dev(flip(z, d), y, core)
        landed(src)
        if ys > 1:
            pass_on(src, y_send.at[d], dev(z, 1 - y, core))
        pass_on(src, s_send.at[d], sib)

    for d in range(1, n):
        src = (me + n - d) % n
        remote(M.at[src], M.at[src], m_send.at[0], m_recv.at[src], sib).wait_recv()
    meta = M[...]
    hit = (meta[:, 0:TOP_K, :] == me.astype(F32)).astype(F32)
    sel = jnp.sum(hit, axis=1)
    weight = jnp.sum(hit * meta[:, TOP_K:2 * TOP_K, :], axis=1)
    before = lax.broadcasted_iota(jnp.int32, (LANES, LANES), 0) <= lax.broadcasted_iota(jnp.int32, (LANES, LANES), 1)
    rank = jnp.dot(sel.astype(BF16), before.astype(F32).astype(BF16), preferred_element_type=F32)
    key = jnp.where(sel > 0.0, rank - 1.0, -1.0)
    per = LANES // rows
    slots = per * cap
    picks, scales = [], []
    for q in range(n // per):
        own = key[q * per:(q + 1) * per]
        place = lax.broadcasted_iota(jnp.int32, (per, cap, LANES), 1).astype(F32)
        pick = (place == own[:, None, :]).astype(F32)
        scale = jnp.sum(pick * weight[q * per:(q + 1) * per][:, None, :], axis=2, keepdims=True)
        picks.append(pick.reshape(slots, LANES))
        scales.append(scale.reshape(slots, 1))
    scale = jnp.concatenate(scales, axis=0)

    if ys > 1:
        for d in range(zs):
            src = dev(flip(z, d), 1 - y, core)
            landed(src)
            pass_on(src, s_send.at[zs + d], sib)
    for d in range(zs):
        for yy in range(ys):
            landed(dev(flip(z, d), yy, 1 - core))

    for q in range(n // per):
        block = G[q * per:(q + 1) * per].reshape(LANES, width)
        X[q * slots:(q + 1) * slots, :] = jnp.dot(
            picks[q].astype(BF16), block, preferred_element_type=F32).astype(BF16)

    for c in loads[:4]:
        c.wait()

    @pl.loop(0, ff // TILE)
    def _(t):
        cols = pl.ds(pl.multiple_of(t * TILE, TILE), TILE)
        gate = jnp.minimum(jnp.dot(X[...], wg[:, cols], preferred_element_type=F32), 7.0)
        upper = jnp.clip(jnp.dot(X[...], wu[:, cols], preferred_element_type=F32), -7.0, 7.0)
        H[:, cols] = (gate * jax.nn.sigmoid(1.702 * gate) * (upper + 1.0)).astype(BF16)

    for c in loads[4:]:
        c.wait()

    def down(base, dst):
        @pl.loop(0, half // TILE)
        def _(t):
            cols = pl.ds(pl.multiple_of(base + t * TILE, TILE), TILE)
            here = pl.ds(pl.multiple_of(t * TILE, TILE), TILE)
            out = jnp.dot(H[...], wd[:, cols], preferred_element_type=F32)
            O[:, here] = (out * scale).astype(BF16)
        for q in range(n // per):
            spread = jnp.dot(picks[q].T.astype(BF16), O[q * slots:(q + 1) * slots, :],
                             preferred_element_type=F32).astype(BF16)
            dst[q * per:(q + 1) * per] = spread.reshape(per, rows, half)

    down((1 - core) * half, Psib)
    first = remote(Psib, R1, r1_send, r1_recv, sib)
    go(first)
    down(core * half, Pown)
    first.wait_recv()

    def pair(zz, yy):
        at = pl.ds(dev(zz, yy, 0), 2)
        return Pown[at].astype(F32) + R1[at].astype(F32)

    order = list(range(zs - 1, -1, -1))
    if ys > 1:
        for d in order:
            Q[d] = pair(flip(z, d), 1 - y).astype(BF16)
            go(remote(Q.at[d], R2.at[d], q_send.at[d], r2_recv.at[d], dev(z, 1 - y, core)))
    final = None
    for d in order:
        total = pair(flip(z, d), y)
        if ys > 1:
            remote(Q.at[d], R2.at[d], q_send.at[d], r2_recv.at[d], sib).wait_recv()
            total = total + R2[d].astype(F32)
        if d:
            T[d] = total.astype(BF16)
            go(remote(T.at[d], R3.at[d], t_send.at[d], r3_recv.at[d], dev(flip(z, d), y, core)))
        else:
            final = total
    for d in order[:-1]:
        remote(T.at[d], R3.at[d], t_send.at[d], r3_recv.at[d], sib).wait_recv()
        final = final + R3[d].astype(F32)
    F4[...] = final.astype(BF16)
    last = remote(F4.at[1 - core], R4, r4_send, r4_recv, sib)
    go(last)
    mine = pl.ds(pl.multiple_of(core * half, half), half)
    other = pl.ds(pl.multiple_of((1 - core) * half, half), half)
    o_ref[:, mine] = F4[core]
    last.wait_recv()
    o_ref[:, other] = R4[...]
    for copy in sends:
        copy.wait_send()


def shards(n, tokens, norm_gain, routes, route_logits, w_gate, w_up, w_down):
    rows, width = tokens.shape
    ff = w_gate.shape[2]
    cap = max(2, 2 * rows * TOP_K // n)
    chips = n // 2
    ys = 2 if chips <= 8 else 1
    zs = chips // ys
    per = LANES // rows
    me = lax.axis_index("ep")
    here = (jnp.arange(LANES) // rows == me % per)[None, :]
    chosen = jnp.where(here, jnp.tile(routes.astype(F32).T, (1, per)), -1.0)
    weights = jnp.where(here, jnp.tile(jax.nn.softmax(route_logits, axis=-1).T, (1, per)), 0.0)
    meta = jnp.concatenate([chosen, weights], axis=0)
    vmem = pl.BlockSpec(memory_space=pltpu.VMEM)
    hbm = pl.BlockSpec(memory_space=pl.ANY)
    half = width // 2
    dma = pltpu.SemaphoreType.DMA
    return pl.pallas_call(
        functools.partial(layer, n, cap, zs, ys),
        out_shape=jax.ShapeDtypeStruct((rows, width), BF16),
        in_specs=[vmem, vmem, vmem, hbm, hbm, hbm],
        out_specs=vmem,
        scratch_shapes=[
            pltpu.VMEM((width, ff), BF16),
            pltpu.VMEM((width, ff), BF16),
            pltpu.VMEM((ff, width), BF16),
            pltpu.VMEM((n, rows, width), BF16),
            pltpu.VMEM((n, 2 * TOP_K, LANES), F32),
            pltpu.VMEM((n * cap, width), BF16),
            pltpu.VMEM((n * cap, ff), BF16),
            pltpu.VMEM((n * cap, half), BF16),
            pltpu.VMEM((n, rows, half), BF16),
            pltpu.VMEM((n, rows, half), BF16),
            pltpu.VMEM((n, rows, half), BF16),
            pltpu.VMEM((zs, 2, rows, half), BF16),
            pltpu.VMEM((zs, 2, rows, half), BF16),
            pltpu.VMEM((zs, 2, rows, half), BF16),
            pltpu.VMEM((zs, 2, rows, half), BF16),
            pltpu.VMEM((2, rows, half), BF16),
            pltpu.VMEM((rows, half), BF16),
            dma((3, 2)), dma((n,)), dma((n,)), dma((zs,)), dma((zs,)), dma((chips,)), dma((n,)),
            dma, dma, dma((zs,)), dma((zs,)), dma((zs,)), dma((zs,)), dma, dma,
        ],
        compiler_params=pltpu.CompilerParams(
            collective_id=0, has_side_effects=True, vmem_limit_bytes=60 * 1024 * 1024),
    )(tokens, norm_gain.reshape(1, width), meta, w_gate, w_up, w_down)


def solution(mesh):
    in_specs = (
        P(("grp", "ep"), None),
        P(),
        P(("grp", "ep"), None),
        P(("grp", "ep"), None),
        P("ep", None, None),
        P("ep", None, None),
        P("ep", None, None),
    )
    out_specs = P(("grp", "ep"), None)
    body = functools.partial(shards, mesh.shape["ep"])
    return jax.shard_map(body, mesh=mesh, in_specs=in_specs, out_specs=out_specs, check_vma=False)
```

```python
import functools

import jax
import jax.numpy as jnp
from jax import lax
from jax.experimental import pallas as pl
from jax.experimental.pallas import tpu as pltpu
from jax.sharding import PartitionSpec as P

TOP_K = 4
LANES = 128
TILE = 256
PARTS = 2
F32 = jnp.float32
BF16 = jnp.bfloat16


def layer(n, cap, zs, ys, x_ref, gain_ref, routes_ref, logits_ref, wg_hbm, wu_hbm, wd_hbm, o_ref,
          wg, wu, wd, G, M, X, H, O, Psib, Pown, R1, Q, R2, T, RZ, acc, F4, R4,
          w_sem, m_send, m_recv, z_send, y_send, s_send, g_recv,
          r1_send, r1_recv, q_send, r2_recv, t_send, rz_recv, r4_send, r4_recv):
    me = lax.axis_index("ep")
    core = me % 2
    chip = me // 2
    z = chip // ys
    y = chip % ys
    sib = chip * 2 + 1 - core
    rows, width = x_ref.shape
    ff = wg.shape[1]
    half = width // 2
    part = half // PARTS
    per = LANES // rows
    slots = per * cap

    def dev(zz, yy, cc):
        return (zz * ys + yy) * 2 + cc

    def remote(src, dst, send, recv, target):
        return pltpu.make_async_remote_copy(
            src_ref=src, dst_ref=dst, send_sem=send, recv_sem=recv,
            device_id={"ep": target}, device_id_type=pl.DeviceIdType.MESH)

    steps = []
    for k in range(1, zs):
        steps.append((2 * k - 1, -k, z >= k))
        steps.append((2 * k, k, z < zs - k))

    loads = []
    for i, (src, dst) in enumerate(((wg_hbm, wg), (wu_hbm, wu), (wd_hbm, wd))):
        k = src.shape[1] // 2
        for h in range(2):
            c = pltpu.make_async_copy(src.at[0, pl.ds(h * k, k)], dst.at[pl.ds(h * k, k)], w_sem.at[i, h])
            c.start()
            loads.append(c)

    x = x_ref[...].astype(F32)
    normed = x * lax.rsqrt(jnp.mean(x * x, axis=-1, keepdims=True) + 1e-06) * gain_ref[...]
    G[me] = normed.astype(BF16)
    spot = (lax.broadcasted_iota(jnp.int32, (rows, LANES), 0) + rows * (me % per)
            == lax.broadcasted_iota(jnp.int32, (rows, LANES), 1)).astype(F32)

    def turned(values):
        return lax.dot_general(values, spot, (((0,), (0,)), ((), ())),
                               precision=lax.Precision.HIGHEST, preferred_element_type=F32)

    logits = logits_ref[...]
    powers = jnp.exp(logits - jnp.max(logits, axis=-1, keepdims=True))
    M[me, 0:TOP_K] = turned((routes_ref[...] + 1).astype(F32))
    M[me, TOP_K:2 * TOP_K] = turned(powers / jnp.sum(powers, axis=-1, keepdims=True))

    barrier = pltpu.get_barrier_semaphore()
    for d in range(1, n):
        pl.semaphore_signal(barrier, inc=1, device_id={"ep": (me + d) % n},
                            device_id_type=pl.DeviceIdType.MESH)
    pl.semaphore_wait(barrier, n - 1)

    sends = []

    def go(copy, there=None):
        if there is None:
            copy.start()
        else:
            pl.when(there)(copy.start)
        sends.append((copy, there))

    def pass_on(src, send, target, there=None):
        go(remote(G.at[src], G.at[src], send, g_recv.at[src], target), there)

    def landed(src):
        remote(G.at[src], G.at[src], z_send.at[0], g_recv.at[src], sib).wait_recv()

    up, down_there = z < zs - 1, z >= 1
    pass_on(me, z_send.at[0], dev(z + 1, y, core), up)
    pass_on(me, z_send.at[2 * zs], dev(z - 1, y, core), down_there)
    if ys > 1:
        pass_on(me, y_send.at[0], dev(z, 1 - y, core))
    pass_on(me, s_send.at[0], sib)
    for d in range(1, n):
        go(remote(M.at[me], M.at[me], m_send.at[d], m_recv.at[me], (me + d) % n))

    for i, k, there in steps:
        src = dev(z + k, y, core)
        pl.when(there)(functools.partial(landed, src))
        if k < 0:
            pass_on(src, z_send.at[i], dev(z + 1, y, core), there & up)
        else:
            pass_on(src, z_send.at[i], dev(z - 1, y, core), there & down_there)
        if ys > 1:
            pass_on(src, y_send.at[i], dev(z, 1 - y, core), there)
        pass_on(src, s_send.at[i], sib, there)

    for d in range(1, n):
        src = (me + n - d) % n
        remote(M.at[src], M.at[src], m_send.at[0], m_recv.at[src], sib).wait_recv()
    meta = M[...]
    hit = (meta[:, 0:TOP_K, :] == (me + 1).astype(F32)).astype(F32)
    sel = jnp.sum(hit, axis=1)
    weight = jnp.sum(hit * meta[:, TOP_K:2 * TOP_K, :], axis=1)
    before = lax.broadcasted_iota(jnp.int32, (LANES, LANES), 0) <= lax.broadcasted_iota(jnp.int32, (LANES, LANES), 1)
    rank = jnp.dot(sel.astype(BF16), before.astype(F32).astype(BF16), preferred_element_type=F32)
    key = jnp.where(sel > 0.0, rank - 1.0, -1.0)
    picks, scales = [], []
    for q in range(n // per):
        own = key[q * per:(q + 1) * per]
        place = lax.broadcasted_iota(jnp.int32, (per, cap, LANES), 1).astype(F32)
        pick = (place == own[:, None, :]).astype(F32)
        scale = jnp.sum(pick * weight[q * per:(q + 1) * per][:, None, :], axis=2, keepdims=True)
        picks.append(pick.reshape(slots, LANES))
        scales.append(scale.reshape(slots, 1))
    scale = jnp.concatenate(scales, axis=0)

    if ys > 1:
        landed(dev(z, 1 - y, core))
        pass_on(dev(z, 1 - y, core), s_send.at[2 * zs], sib)
        for i, k, there in steps:
            src = dev(z + k, 1 - y, core)
            pl.when(there)(functools.partial(landed, src))
            pass_on(src, s_send.at[2 * zs + i], sib, there)
    for yy in range(ys):
        landed(dev(z, yy, 1 - core))
        for i, k, there in steps:
            pl.when(there)(functools.partial(landed, dev(z + k, yy, 1 - core)))

    for q in range(n // per):
        block = G[q * per:(q + 1) * per].reshape(LANES, width)
        X[q * slots:(q + 1) * slots, :] = jnp.dot(
            picks[q].astype(BF16), block, preferred_element_type=F32).astype(BF16)

    for c in loads[:4]:
        c.wait()

    @pl.loop(0, ff // TILE)
    def _(t):
        cols = pl.ds(pl.multiple_of(t * TILE, TILE), TILE)
        gate = jnp.minimum(jnp.dot(X[...], wg[:, cols], preferred_element_type=F32), 7.0)
        upper = jnp.clip(jnp.dot(X[...], wu[:, cols], preferred_element_type=F32), -7.0, 7.0)
        H[:, cols] = (gate * jax.nn.sigmoid(1.702 * gate) * (upper + 1.0)).astype(BF16)

    for c in loads[4:]:
        c.wait()

    def down(base, dst):
        @pl.loop(0, part // TILE)
        def _(t):
            cols = pl.ds(pl.multiple_of(base + t * TILE, TILE), TILE)
            here = pl.ds(pl.multiple_of(t * TILE, TILE), TILE)
            out = jnp.dot(H[...], wd[:, cols], preferred_element_type=F32)
            O[:, here] = (out * scale).astype(BF16)
        for q in range(n // per):
            spread = jnp.dot(picks[q].T.astype(BF16), O[q * slots:(q + 1) * slots, :],
                             preferred_element_type=F32).astype(BF16)
            dst[q * per:(q + 1) * per] = spread.reshape(per, rows, part)

    def pair(p, zz, yy):
        at = pl.ds(dev(zz, yy, 0), 2)
        return Pown[p, at].astype(F32) + R1[p, at].astype(F32)

    far = steps[::-1]

    def to_core(p):
        down((1 - core) * half + p * part, Psib.at[p])
        go(remote(Psib.at[p], R1.at[p], r1_send.at[p], r1_recv.at[p], sib))

    def to_y(p):
        remote(Psib.at[p], R1.at[p], r1_send.at[p], r1_recv.at[p], sib).wait_recv()
        if ys > 1:
            for i, k, there in far + [(0, 0, None)]:
                def put(i=i, k=k):
                    Q[p, i] = pair(p, z + k, 1 - y).astype(BF16)
                if there is None:
                    put()
                else:
                    pl.when(there)(put)
                go(remote(Q.at[p, i], R2.at[p, i], q_send.at[p, i], r2_recv.at[p, i], dev(z, 1 - y, core)), there)

    def gathered(p, i, k):
        total = pair(p, z + k, y)
        if ys > 1:
            remote(Q.at[p, i], R2.at[p, i], q_send.at[p, i], r2_recv.at[p, i], sib).wait_recv()
            total = total + R2[p, i].astype(F32)
        return total

    def take(p, i):
        remote(T.at[p, i], RZ.at[p, i], t_send.at[p, i], rz_recv.at[p, i], sib).wait_recv()
        acc[...] += RZ[p, i].astype(F32)

    def to_z(p):
        for i, k, there in far:
            def put(i=i, k=k):
                acc[...] = gathered(p, i, k)
                if k > 0 and k < zs - 1:
                    pl.when(down_there)(functools.partial(take, p, i + 2))
                if k < 0 and k > 1 - zs:
                    pl.when(up)(functools.partial(take, p, i + 2))
                T[p, i] = acc[...].astype(BF16)
            pl.when(there)(put)
            target = dev(z + 1, y, core) if k > 0 else dev(z - 1, y, core)
            go(remote(T.at[p, i], RZ.at[p, i], t_send.at[p, i], rz_recv.at[p, i], target), there)

    def to_end(p):
        acc[...] = gathered(p, 0, 0)
        if zs > 1:
            pl.when(down_there)(functools.partial(take, p, 2))
            pl.when(up)(functools.partial(take, p, 1))
        F4[p] = acc[...].astype(BF16)
        go(remote(F4.at[p, 1 - core], R4.at[p], r4_send.at[p], r4_recv.at[p], sib))

    to_core(0)
    down(core * half, Pown.at[0])
    for p in range(1, PARTS):
        to_core(p)
        to_y(p - 1)
        down(core * half + p * part, Pown.at[p])
    to_y(PARTS - 1)
    to_z(0)
    for p in range(1, PARTS):
        to_z(p)
    for p in range(PARTS):
        to_end(p)
    for p in range(PARTS):
        o_ref[:, pl.ds(pl.multiple_of(core * half + p * part, part), part)] = F4[p, core]
    for p in range(PARTS):
        remote(F4.at[p, 1 - core], R4.at[p], r4_send.at[p], r4_recv.at[p], sib).wait_recv()
        o_ref[:, pl.ds(pl.multiple_of((1 - core) * half + p * part, part), part)] = R4[p]
    for copy, there in sends:
        if there is None:
            copy.wait_send()
        else:
            pl.when(there)(copy.wait_send)


def shards(n, tokens, norm_gain, routes, route_logits, w_gate, w_up, w_down):
    rows, width = tokens.shape
    ff = w_gate.shape[2]
    cap = max(2, 2 * rows * TOP_K // n)
    chips = n // 2
    ys = 2 if chips <= 8 else 1
    zs = chips // ys
    vmem = pl.BlockSpec(memory_space=pltpu.VMEM)
    hbm = pl.BlockSpec(memory_space=pl.ANY)
    part = width // 2 // PARTS
    dma = pltpu.SemaphoreType.DMA
    side = pltpu.VMEM((PARTS, n, rows, part), BF16)
    line = pltpu.VMEM((PARTS, 2 * zs - 1, 2, rows, part), BF16)
    return pl.pallas_call(
        functools.partial(layer, n, cap, zs, ys),
        out_shape=jax.ShapeDtypeStruct((rows, width), BF16),
        in_specs=[vmem, vmem, vmem, vmem, hbm, hbm, hbm],
        out_specs=vmem,
        scratch_shapes=[
            pltpu.VMEM((width, ff), BF16),
            pltpu.VMEM((width, ff), BF16),
            pltpu.VMEM((ff, width), BF16),
            pltpu.VMEM((n, rows, width), BF16),
            pltpu.VMEM((n, 2 * TOP_K, LANES), F32),
            pltpu.VMEM((n * cap, width), BF16),
            pltpu.VMEM((n * cap, ff), BF16),
            pltpu.VMEM((n * cap, part), BF16),
            side, side, side, line, line, line, line,
            pltpu.VMEM((2, rows, part), F32),
            pltpu.VMEM((PARTS, 2, rows, part), BF16),
            pltpu.VMEM((PARTS, rows, part), BF16),
            dma((3, 2)), dma((n,)), dma((n,)), dma((2 * zs + 1,)), dma((2 * zs,)), dma((4 * zs,)), dma((n,)),
            dma((PARTS,)), dma((PARTS,)), dma((PARTS, 2 * zs)), dma((PARTS, 2 * zs)),
            dma((PARTS, 2 * zs)), dma((PARTS, 2 * zs)), dma((PARTS,)), dma((PARTS,)),
        ],
        compiler_params=pltpu.CompilerParams(
            collective_id=0, has_side_effects=True, vmem_limit_bytes=60 * 1024 * 1024),
    )(tokens, norm_gain.reshape(1, width), routes, route_logits, w_gate, w_up, w_down)


def solution(mesh):
    in_specs = (
        P(("grp", "ep"), None),
        P(),
        P(("grp", "ep"), None),
        P(("grp", "ep"), None),
        P("ep", None, None),
        P("ep", None, None),
        P("ep", None, None),
    )
    out_specs = P(("grp", "ep"), None)
    body = functools.partial(shards, mesh.shape["ep"])
    return jax.shard_map(body, mesh=mesh, in_specs=in_specs, out_specs=out_specs, check_vma=False)
```

```python
import functools

import jax
import jax.numpy as jnp
from jax import lax
from jax.experimental import pallas as pl
from jax.experimental.pallas import tpu as pltpu
from jax.sharding import PartitionSpec as P

TOP_K = 4
LANES = 128
TILE = 256
PARTS = 2
SPLIT = 2
F32 = jnp.float32
BF16 = jnp.bfloat16


def layer(n, cap, zs, ys, x_ref, gain_ref, routes_ref, logits_ref, wg_hbm, wu_hbm, wd_hbm, o_ref,
          wg, wu, wd, G, M, X, H, O, Psib, Pown, R1, Q, R2, T, RZ, acc, F4, R4,
          w_sem, m_send, m_recv, z_send, y_send, s_send, g_recv,
          r1_send, r1_recv, q_send, r2_recv, t_send, rz_recv, r4_send, r4_recv):
    me = lax.axis_index("ep")
    core = me % 2
    chip = me // 2
    z = chip // ys
    y = chip % ys
    sib = chip * 2 + 1 - core
    rows, width = x_ref.shape
    ff = wg.shape[1]
    half = width // 2
    part = half // PARTS
    per = LANES // rows
    slots = per * cap

    def dev(zz, yy, cc):
        return (zz * ys + yy) * 2 + cc

    def remote(src, dst, send, recv, target):
        return pltpu.make_async_remote_copy(
            src_ref=src, dst_ref=dst, send_sem=send, recv_sem=recv,
            device_id={"ep": target}, device_id_type=pl.DeviceIdType.MESH)

    steps = []
    for k in range(1, zs):
        steps.append((2 * k - 1, -k, z >= k))
        steps.append((2 * k, k, z < zs - k))

    loads = []
    for i, (src, dst) in enumerate(((wg_hbm, wg), (wu_hbm, wu), (wd_hbm, wd))):
        k = src.shape[1] // 2
        for h in range(2):
            c = pltpu.make_async_copy(src.at[0, pl.ds(h * k, k)], dst.at[pl.ds(h * k, k)], w_sem.at[i, h])
            c.start()
            loads.append(c)

    x = x_ref[...].astype(F32)
    normed = x * lax.rsqrt(jnp.mean(x * x, axis=-1, keepdims=True) + 1e-06) * gain_ref[...]
    G[me] = normed.astype(BF16)
    spot = (lax.broadcasted_iota(jnp.int32, (rows, LANES), 0) + rows * (me % per)
            == lax.broadcasted_iota(jnp.int32, (rows, LANES), 1)).astype(F32)

    def placed(values):
        return jnp.dot(values, spot, precision=lax.Precision.HIGHEST, preferred_element_type=F32)

    logits = logits_ref[...]
    powers = jnp.exp(logits - jnp.max(logits, axis=0, keepdims=True))
    M[me, 0:TOP_K] = placed((routes_ref[...] + 1).astype(F32))
    M[me, TOP_K:2 * TOP_K] = placed(powers / jnp.sum(powers, axis=0, keepdims=True))

    barrier = pltpu.get_barrier_semaphore()
    for d in range(1, n):
        pl.semaphore_signal(barrier, inc=1, device_id={"ep": (me + d) % n},
                            device_id_type=pl.DeviceIdType.MESH)
    pl.semaphore_wait(barrier, n - 1)

    sends = []

    def go(copy, there=None):
        if there is None:
            copy.start()
        else:
            pl.when(there)(copy.start)
        sends.append((copy, there))

    def piece(src, h):
        return G.at[src, pl.ds(h * (rows // SPLIT), rows // SPLIT)]

    def pass_on(src, h, send, i, target, there=None):
        go(remote(piece(src, h), piece(src, h), send.at[i, h], g_recv.at[src, h], target), there)

    def landed(src, h):
        remote(piece(src, h), piece(src, h), z_send.at[0, h], g_recv.at[src, h], sib).wait_recv()

    up, down_there = z < zs - 1, z >= 1
    for h in range(SPLIT):
        pass_on(me, h, z_send, 0, dev(z + 1, y, core), up)
        pass_on(me, h, z_send, 2 * zs, dev(z - 1, y, core), down_there)
        if ys > 1:
            pass_on(me, h, y_send, 0, dev(z, 1 - y, core))
        pass_on(me, h, s_send, 0, sib)
    for d in range(1, n):
        go(remote(M.at[me], M.at[me], m_send.at[d], m_recv.at[me], (me + d) % n))

    def from_z(i, k, there):
        src = dev(z + k, y, core)
        for h in range(SPLIT):
            pl.when(there)(functools.partial(landed, src, h))
            if k < 0:
                pass_on(src, h, z_send, i, dev(z + 1, y, core), there & up)
            else:
                pass_on(src, h, z_send, i, dev(z - 1, y, core), there & down_there)
            if ys > 1:
                pass_on(src, h, y_send, i, dev(z, 1 - y, core), there)
            pass_on(src, h, s_send, i, sib, there)

    def from_y(i, k, there):
        src = dev(z + k, 1 - y, core)
        for h in range(SPLIT):
            if there is None:
                landed(src, h)
            else:
                pl.when(there)(functools.partial(landed, src, h))
            pass_on(src, h, s_send, 2 * zs + i, sib, there)

    late = [(0, 0, None)] + steps
    for j in range(0, len(steps), 2):
        for step in steps[j:j + 2]:
            from_z(*step)
        if ys > 1:
            for step in late[max(0, j - 1):j + 1]:
                from_y(*step)

    for d in range(1, n):
        src = (me + n - d) % n
        remote(M.at[src], M.at[src], m_send.at[0], m_recv.at[src], sib).wait_recv()
    meta = M[...]
    hit = (meta[:, 0:TOP_K, :] == (me + 1).astype(F32)).astype(F32)
    sel = jnp.sum(hit, axis=1)
    weight = jnp.sum(hit * meta[:, TOP_K:2 * TOP_K, :], axis=1)
    before = lax.broadcasted_iota(jnp.int32, (LANES, LANES), 0) <= lax.broadcasted_iota(jnp.int32, (LANES, LANES), 1)
    rank = jnp.dot(sel.astype(BF16), before.astype(F32).astype(BF16), preferred_element_type=F32)
    key = jnp.where(sel > 0.0, rank - 1.0, -1.0)
    picks, scales = [], []
    for q in range(n // per):
        own = key[q * per:(q + 1) * per]
        place = lax.broadcasted_iota(jnp.int32, (per, cap, LANES), 1).astype(F32)
        pick = (place == own[:, None, :]).astype(F32)
        scale = jnp.sum(pick * weight[q * per:(q + 1) * per][:, None, :], axis=2, keepdims=True)
        picks.append(pick.reshape(slots, LANES))
        scales.append(scale.reshape(slots, 1))
    scale = jnp.concatenate(scales, axis=0)

    if ys > 1:
        for step in late[max(0, len(steps) - 1):]:
            from_y(*step)
    for yy in range(ys):
        for h in range(SPLIT):
            landed(dev(z, yy, 1 - core), h)
            for i, k, there in steps:
                pl.when(there)(functools.partial(landed, dev(z + k, yy, 1 - core), h))

    for q in range(n // per):
        block = G[q * per:(q + 1) * per].reshape(LANES, width)
        X[q * slots:(q + 1) * slots, :] = jnp.dot(
            picks[q].astype(BF16), block, preferred_element_type=F32).astype(BF16)

    for c in loads[:4]:
        c.wait()

    @pl.loop(0, ff // TILE)
    def _(t):
        cols = pl.ds(pl.multiple_of(t * TILE, TILE), TILE)
        gate = jnp.minimum(jnp.dot(X[...], wg[:, cols], preferred_element_type=F32), 7.0)
        upper = jnp.clip(jnp.dot(X[...], wu[:, cols], preferred_element_type=F32), -7.0, 7.0)
        H[:, cols] = (gate * jax.nn.sigmoid(1.702 * gate) * (upper + 1.0)).astype(BF16)

    for c in loads[4:]:
        c.wait()

    def down(base, dst):
        @pl.loop(0, part // TILE)
        def _(t):
            cols = pl.ds(pl.multiple_of(base + t * TILE, TILE), TILE)
            here = pl.ds(pl.multiple_of(t * TILE, TILE), TILE)
            out = jnp.dot(H[...], wd[:, cols], preferred_element_type=F32)
            O[:, here] = (out * scale).astype(BF16)
        for q in range(n // per):
            spread = jnp.dot(picks[q].T.astype(BF16), O[q * slots:(q + 1) * slots, :],
                             preferred_element_type=F32).astype(BF16)
            dst[q * per:(q + 1) * per] = spread.reshape(per, rows, part)

    def pair(p, zz, yy):
        at = pl.ds(dev(zz, yy, 0), 2)
        return Pown[p, at].astype(F32) + R1[p, at].astype(F32)

    far = steps[::-1]

    def to_core(p):
        down((1 - core) * half + p * part, Psib.at[p])
        go(remote(Psib.at[p], R1.at[p], r1_send.at[p], r1_recv.at[p], sib))

    def to_y(p):
        remote(Psib.at[p], R1.at[p], r1_send.at[p], r1_recv.at[p], sib).wait_recv()
        if ys > 1:
            for i, k, there in far + [(0, 0, None)]:
                def put(i=i, k=k):
                    Q[p, i] = pair(p, z + k, 1 - y).astype(BF16)
                if there is None:
                    put()
                else:
                    pl.when(there)(put)
                go(remote(Q.at[p, i], R2.at[p, i], q_send.at[p, i], r2_recv.at[p, i], dev(z, 1 - y, core)), there)

    def gathered(p, i, k):
        total = pair(p, z + k, y)
        if ys > 1:
            remote(Q.at[p, i], R2.at[p, i], q_send.at[p, i], r2_recv.at[p, i], sib).wait_recv()
            total = total + R2[p, i].astype(F32)
        return total

    def take(p, i):
        remote(T.at[p, i], RZ.at[p, i], t_send.at[p, i], rz_recv.at[p, i], sib).wait_recv()
        acc[...] += RZ[p, i].astype(F32)

    def to_z(p):
        for i, k, there in far:
            def put(i=i, k=k):
                acc[...] = gathered(p, i, k)
                if k > 0 and k < zs - 1:
                    pl.when(down_there)(functools.partial(take, p, i + 2))
                if k < 0 and k > 1 - zs:
                    pl.when(up)(functools.partial(take, p, i + 2))
                T[p, i] = acc[...].astype(BF16)
            pl.when(there)(put)
            target = dev(z + 1, y, core) if k > 0 else dev(z - 1, y, core)
            go(remote(T.at[p, i], RZ.at[p, i], t_send.at[p, i], rz_recv.at[p, i], target), there)

    def to_end(p):
        acc[...] = gathered(p, 0, 0)
        if zs > 1:
            pl.when(down_there)(functools.partial(take, p, 2))
            pl.when(up)(functools.partial(take, p, 1))
        F4[p] = acc[...].astype(BF16)
        go(remote(F4.at[p, 1 - core], R4.at[p], r4_send.at[p], r4_recv.at[p], sib))

    to_core(0)
    down(core * half, Pown.at[0])
    for p in range(1, PARTS):
        to_core(p)
        to_y(p - 1)
        down(core * half + p * part, Pown.at[p])
    to_y(PARTS - 1)
    to_z(0)
    for p in range(1, PARTS):
        to_z(p)
    for p in range(PARTS):
        to_end(p)
    for p in range(PARTS):
        o_ref[:, pl.ds(pl.multiple_of(core * half + p * part, part), part)] = F4[p, core]
    for p in range(PARTS):
        remote(F4.at[p, 1 - core], R4.at[p], r4_send.at[p], r4_recv.at[p], sib).wait_recv()
        o_ref[:, pl.ds(pl.multiple_of((1 - core) * half + p * part, part), part)] = R4[p]
    for copy, there in sends:
        if there is None:
            copy.wait_send()
        else:
            pl.when(there)(copy.wait_send)


def shards(n, tokens, norm_gain, routes, route_logits, w_gate, w_up, w_down):
    rows, width = tokens.shape
    ff = w_gate.shape[2]
    cap = max(2, 2 * rows * TOP_K // n)
    chips = n // 2
    ys = 2 if chips <= 8 else 1
    zs = chips // ys
    vmem = pl.BlockSpec(memory_space=pltpu.VMEM)
    hbm = pl.BlockSpec(memory_space=pl.ANY)
    part = width // 2 // PARTS
    dma = pltpu.SemaphoreType.DMA
    side = pltpu.VMEM((PARTS, n, rows, part), BF16)
    line = pltpu.VMEM((PARTS, 2 * zs - 1, 2, rows, part), BF16)
    return pl.pallas_call(
        functools.partial(layer, n, cap, zs, ys),
        out_shape=jax.ShapeDtypeStruct((rows, width), BF16),
        in_specs=[vmem, vmem, vmem, vmem, hbm, hbm, hbm],
        out_specs=vmem,
        scratch_shapes=[
            pltpu.VMEM((width, ff), BF16),
            pltpu.VMEM((width, ff), BF16),
            pltpu.VMEM((ff, width), BF16),
            pltpu.VMEM((n, rows, width), BF16),
            pltpu.VMEM((n, 2 * TOP_K, LANES), F32),
            pltpu.VMEM((n * cap, width), BF16),
            pltpu.VMEM((n * cap, ff), BF16),
            pltpu.VMEM((n * cap, part), BF16),
            side, side, side, line, line, line, line,
            pltpu.VMEM((2, rows, part), F32),
            pltpu.VMEM((PARTS, 2, rows, part), BF16),
            pltpu.VMEM((PARTS, rows, part), BF16),
            dma((3, 2)), dma((n,)), dma((n,)), dma((2 * zs + 1, SPLIT)), dma((2 * zs, SPLIT)), dma((4 * zs, SPLIT)),
            dma((n, SPLIT)),
            dma((PARTS,)), dma((PARTS,)), dma((PARTS, 2 * zs)), dma((PARTS, 2 * zs)),
            dma((PARTS, 2 * zs)), dma((PARTS, 2 * zs)), dma((PARTS,)), dma((PARTS,)),
        ],
        compiler_params=pltpu.CompilerParams(
            collective_id=0, has_side_effects=True, vmem_limit_bytes=60 * 1024 * 1024),
    )(tokens, norm_gain.reshape(1, width), routes.T, route_logits.T, w_gate, w_up, w_down)


def solution(mesh):
    in_specs = (
        P(("grp", "ep"), None),
        P(),
        P(("grp", "ep"), None),
        P(("grp", "ep"), None),
        P("ep", None, None),
        P("ep", None, None),
        P("ep", None, None),
    )
    out_specs = P(("grp", "ep"), None)
    body = functools.partial(shards, mesh.shape["ep"])
    return jax.shard_map(body, mesh=mesh, in_specs=in_specs, out_specs=out_specs, check_vma=False)
```

```python
import functools

import jax
import jax.numpy as jnp
from jax import lax
from jax.experimental import pallas as pl
from jax.experimental.pallas import tpu as pltpu
from jax.sharding import PartitionSpec as P

TOP_K = 4
LANES = 128
TILE = 256
PARTS = 2
SPLIT = 2
F32 = jnp.float32
BF16 = jnp.bfloat16


def layer(n, cap, zs, ys, x_ref, gain_ref, routes_ref, logits_ref, wg_hbm, wu_hbm, wd_hbm, o_ref,
          wg, wu, wd, G, M, X, H, O, Psib, Pown, R1, Q, R2, T, RZ, acc, F4, R4,
          w_sem, m_send, m_recv, z_send, y_send, s_send, g_recv,
          r1_send, r1_recv, q_send, r2_recv, t_send, rz_recv, r4_send, r4_recv):
    me = lax.axis_index("ep")
    core = me % 2
    chip = me // 2
    z = chip // ys
    y = chip % ys
    sib = chip * 2 + 1 - core
    rows, width = x_ref.shape
    ff = wg.shape[1]
    half = width // 2
    part = half // PARTS
    per = LANES // rows
    slots = per * cap

    def dev(zz, yy, cc):
        return (zz * ys + yy) * 2 + cc

    def remote(src, dst, send, recv, target):
        return pltpu.make_async_remote_copy(
            src_ref=src, dst_ref=dst, send_sem=send, recv_sem=recv,
            device_id={"ep": target}, device_id_type=pl.DeviceIdType.MESH)

    steps = []
    for k in range(1, zs):
        steps.append((2 * k - 1, -k, z >= k))
        steps.append((2 * k, k, z < zs - k))

    loads = []
    for i, (src, dst) in enumerate(((wg_hbm, wg), (wu_hbm, wu), (wd_hbm, wd))):
        k = src.shape[1] // 2
        for h in range(2):
            c = pltpu.make_async_copy(src.at[0, pl.ds(h * k, k)], dst.at[pl.ds(h * k, k)], w_sem.at[i, h])
            c.start()
            loads.append(c)

    x = x_ref[...].astype(F32)
    normed = x * lax.rsqrt(jnp.mean(x * x, axis=-1, keepdims=True) + 1e-06) * gain_ref[...]
    G[me] = normed.astype(BF16)
    spot = (lax.broadcasted_iota(jnp.int32, (rows, LANES), 0) + rows * (me % per)
            == lax.broadcasted_iota(jnp.int32, (rows, LANES), 1)).astype(F32)

    def placed(values):
        return jnp.dot(values, spot, precision=lax.Precision.HIGHEST, preferred_element_type=F32)

    logits = logits_ref[...]
    powers = jnp.exp(logits - jnp.max(logits, axis=0, keepdims=True))
    M[me, 0:TOP_K] = placed((routes_ref[...] + 1).astype(F32))
    M[me, TOP_K:2 * TOP_K] = placed(powers / jnp.sum(powers, axis=0, keepdims=True))

    barrier = pltpu.get_barrier_semaphore()
    for d in range(1, n):
        pl.semaphore_signal(barrier, inc=1, device_id={"ep": (me + d) % n},
                            device_id_type=pl.DeviceIdType.MESH)
    pl.semaphore_wait(barrier, n - 1)

    sends = []

    def go(copy, there=None):
        if there is None:
            copy.start()
        else:
            pl.when(there)(copy.start)
        sends.append((copy, there))

    def piece(src, h):
        return G.at[src, pl.ds(h * (rows // SPLIT), rows // SPLIT)]

    def pass_on(src, h, send, i, target, there=None):
        go(remote(piece(src, h), piece(src, h), send.at[i, h], g_recv.at[src, h], target), there)

    def landed(src, h):
        remote(piece(src, h), piece(src, h), z_send.at[0, h], g_recv.at[src, h], sib).wait_recv()

    up, down_there = z < zs - 1, z >= 1
    for h in range(SPLIT):
        pass_on(me, h, z_send, 0, dev(z + 1, y, core), up)
        pass_on(me, h, z_send, 2 * zs, dev(z - 1, y, core), down_there)
        if ys > 1:
            pass_on(me, h, y_send, 0, dev(z, 1 - y, core))
        pass_on(me, h, s_send, 0, sib)
    for d in range(1, n):
        go(remote(M.at[me], M.at[me], m_send.at[d], m_recv.at[me], (me + d) % n))

    def from_z(i, k, there):
        src = dev(z + k, y, core)
        for h in range(SPLIT):
            pl.when(there)(functools.partial(landed, src, h))
            if k < 0:
                pass_on(src, h, z_send, i, dev(z + 1, y, core), there & up)
            else:
                pass_on(src, h, z_send, i, dev(z - 1, y, core), there & down_there)
            if ys > 1:
                pass_on(src, h, y_send, i, dev(z, 1 - y, core), there)
            pass_on(src, h, s_send, i, sib, there)

    def from_y(i, k, there):
        src = dev(z + k, 1 - y, core)
        for h in range(SPLIT):
            if there is None:
                landed(src, h)
            else:
                pl.when(there)(functools.partial(landed, src, h))
            pass_on(src, h, s_send, 2 * zs + i, sib, there)

    late = [(0, 0, None)] + steps
    for j in range(0, len(steps), 2):
        for step in steps[j:j + 2]:
            from_z(*step)
        if ys > 1:
            for step in late[max(0, j - 1):j + 1]:
                from_y(*step)

    for d in range(1, n):
        src = (me + n - d) % n
        remote(M.at[src], M.at[src], m_send.at[0], m_recv.at[src], sib).wait_recv()
    meta = M[...]
    hit = (meta[:, 0:TOP_K, :] == (me + 1).astype(F32)).astype(F32)
    sel = jnp.sum(hit, axis=1)
    weight = jnp.sum(hit * meta[:, TOP_K:2 * TOP_K, :], axis=1)
    before = lax.broadcasted_iota(jnp.int32, (LANES, LANES), 0) <= lax.broadcasted_iota(jnp.int32, (LANES, LANES), 1)
    rank = jnp.dot(sel.astype(BF16), before.astype(F32).astype(BF16), preferred_element_type=F32)
    key = jnp.where(sel > 0.0, rank - 1.0, -1.0)
    picks, scales = [], []
    for q in range(n // per):
        own = key[q * per:(q + 1) * per]
        place = lax.broadcasted_iota(jnp.int32, (per, cap, LANES), 1).astype(F32)
        pick = (place == own[:, None, :]).astype(F32)
        scale = jnp.sum(pick * weight[q * per:(q + 1) * per][:, None, :], axis=2, keepdims=True)
        picks.append(pick.reshape(slots, LANES))
        scales.append(scale.reshape(slots, 1))
    scale = jnp.concatenate(scales, axis=0)

    if ys > 1:
        for step in late[max(0, len(steps) - 1):]:
            from_y(*step)
    for yy in range(ys):
        for h in range(SPLIT):
            landed(dev(z, yy, 1 - core), h)
            for i, k, there in steps:
                pl.when(there)(functools.partial(landed, dev(z + k, yy, 1 - core), h))

    for q in range(n // per):
        block = G[q * per:(q + 1) * per].reshape(LANES, width)
        X[q * slots:(q + 1) * slots, :] = jnp.dot(
            picks[q].astype(BF16), block, preferred_element_type=F32).astype(BF16)

    for c in loads[:4]:
        c.wait()

    @pl.loop(0, ff // TILE, unroll=True)
    def _(t):
        cols = pl.ds(pl.multiple_of(t * TILE, TILE), TILE)
        gate = jnp.minimum(jnp.dot(X[...], wg[:, cols], preferred_element_type=F32), 7.0)
        upper = jnp.clip(jnp.dot(X[...], wu[:, cols], preferred_element_type=F32), -7.0, 7.0)
        H[:, cols] = (gate * jax.nn.sigmoid(1.702 * gate) * (upper + 1.0)).astype(BF16)

    for c in loads[4:]:
        c.wait()

    def down(base, dst):
        @pl.loop(0, part // TILE, unroll=True)
        def _(t):
            cols = pl.ds(pl.multiple_of(base + t * TILE, TILE), TILE)
            here = pl.ds(pl.multiple_of(t * TILE, TILE), TILE)
            out = jnp.dot(H[...], wd[:, cols], preferred_element_type=F32)
            O[:, here] = (out * scale).astype(BF16)
        for q in range(n // per):
            spread = jnp.dot(picks[q].T.astype(BF16), O[q * slots:(q + 1) * slots, :],
                             preferred_element_type=F32).astype(BF16)
            dst[q * per:(q + 1) * per] = spread.reshape(per, rows, part)

    def pair(p, zz, yy):
        at = pl.ds(dev(zz, yy, 0), 2)
        return Pown[p, at].astype(F32) + R1[p, at].astype(F32)

    far = steps[::-1]

    def to_core(p):
        down((1 - core) * half + p * part, Psib.at[p])
        go(remote(Psib.at[p], R1.at[p], r1_send.at[p], r1_recv.at[p], sib))

    def to_y(p):
        remote(Psib.at[p], R1.at[p], r1_send.at[p], r1_recv.at[p], sib).wait_recv()
        if ys > 1:
            for i, k, there in far + [(0, 0, None)]:
                def put(i=i, k=k):
                    Q[p, i] = pair(p, z + k, 1 - y).astype(BF16)
                if there is None:
                    put()
                else:
                    pl.when(there)(put)
                go(remote(Q.at[p, i], R2.at[p, i], q_send.at[p, i], r2_recv.at[p, i], dev(z, 1 - y, core)), there)

    def gathered(p, i, k):
        total = pair(p, z + k, y)
        if ys > 1:
            remote(Q.at[p, i], R2.at[p, i], q_send.at[p, i], r2_recv.at[p, i], sib).wait_recv()
            total = total + R2[p, i].astype(F32)
        return total

    def take(p, i):
        remote(T.at[p, i], RZ.at[p, i], t_send.at[p, i], rz_recv.at[p, i], sib).wait_recv()
        acc[...] += RZ[p, i].astype(F32)

    def to_z(p):
        for i, k, there in far:
            def put(i=i, k=k):
                acc[...] = gathered(p, i, k)
                if k > 0 and k < zs - 1:
                    pl.when(down_there)(functools.partial(take, p, i + 2))
                if k < 0 and k > 1 - zs:
                    pl.when(up)(functools.partial(take, p, i + 2))
                T[p, i] = acc[...].astype(BF16)
            pl.when(there)(put)
            target = dev(z + 1, y, core) if k > 0 else dev(z - 1, y, core)
            go(remote(T.at[p, i], RZ.at[p, i], t_send.at[p, i], rz_recv.at[p, i], target), there)

    def to_end(p):
        acc[...] = gathered(p, 0, 0)
        if zs > 1:
            pl.when(down_there)(functools.partial(take, p, 2))
            pl.when(up)(functools.partial(take, p, 1))
        F4[p] = acc[...].astype(BF16)
        go(remote(F4.at[p, 1 - core], R4.at[p], r4_send.at[p], r4_recv.at[p], sib))

    to_core(0)
    down(core * half, Pown.at[0])
    for p in range(1, PARTS):
        to_core(p)
        to_y(p - 1)
        down(core * half + p * part, Pown.at[p])
    to_y(PARTS - 1)
    to_z(0)
    for p in range(1, PARTS):
        to_z(p)
    for p in range(PARTS):
        to_end(p)
    for p in range(PARTS):
        o_ref[:, pl.ds(pl.multiple_of(core * half + p * part, part), part)] = F4[p, core]
    for p in range(PARTS):
        remote(F4.at[p, 1 - core], R4.at[p], r4_send.at[p], r4_recv.at[p], sib).wait_recv()
        o_ref[:, pl.ds(pl.multiple_of((1 - core) * half + p * part, part), part)] = R4[p]
    for copy, there in sends:
        if there is None:
            copy.wait_send()
        else:
            pl.when(there)(copy.wait_send)


def shards(n, tokens, norm_gain, routes, route_logits, w_gate, w_up, w_down):
    rows, width = tokens.shape
    ff = w_gate.shape[2]
    cap = max(2, 2 * rows * TOP_K // n)
    chips = n // 2
    ys = 2 if chips <= 8 else 1
    zs = chips // ys
    vmem = pl.BlockSpec(memory_space=pltpu.VMEM)
    hbm = pl.BlockSpec(memory_space=pl.ANY)
    part = width // 2 // PARTS
    dma = pltpu.SemaphoreType.DMA
    side = pltpu.VMEM((PARTS, n, rows, part), BF16)
    line = pltpu.VMEM((PARTS, 2 * zs - 1, 2, rows, part), BF16)
    return pl.pallas_call(
        functools.partial(layer, n, cap, zs, ys),
        out_shape=jax.ShapeDtypeStruct((rows, width), BF16),
        in_specs=[vmem, vmem, vmem, vmem, hbm, hbm, hbm],
        out_specs=vmem,
        scratch_shapes=[
            pltpu.VMEM((width, ff), BF16),
            pltpu.VMEM((width, ff), BF16),
            pltpu.VMEM((ff, width), BF16),
            pltpu.VMEM((n, rows, width), BF16),
            pltpu.VMEM((n, 2 * TOP_K, LANES), F32),
            pltpu.VMEM((n * cap, width), BF16),
            pltpu.VMEM((n * cap, ff), BF16),
            pltpu.VMEM((n * cap, part), BF16),
            side, side, side, line, line, line, line,
            pltpu.VMEM((2, rows, part), F32),
            pltpu.VMEM((PARTS, 2, rows, part), BF16),
            pltpu.VMEM((PARTS, rows, part), BF16),
            dma((3, 2)), dma((n,)), dma((n,)), dma((2 * zs + 1, SPLIT)), dma((2 * zs, SPLIT)), dma((4 * zs, SPLIT)),
            dma((n, SPLIT)),
            dma((PARTS,)), dma((PARTS,)), dma((PARTS, 2 * zs)), dma((PARTS, 2 * zs)),
            dma((PARTS, 2 * zs)), dma((PARTS, 2 * zs)), dma((PARTS,)), dma((PARTS,)),
        ],
        compiler_params=pltpu.CompilerParams(
            collective_id=0, has_side_effects=True, vmem_limit_bytes=60 * 1024 * 1024),
    )(tokens, norm_gain.reshape(1, width), routes.T, route_logits.T, w_gate, w_up, w_down)


def solution(mesh):
    in_specs = (
        P(("grp", "ep"), None),
        P(),
        P(("grp", "ep"), None),
        P(("grp", "ep"), None),
        P("ep", None, None),
        P("ep", None, None),
        P("ep", None, None),
    )
    out_specs = P(("grp", "ep"), None)
    body = functools.partial(shards, mesh.shape["ep"])
    return jax.shard_map(body, mesh=mesh, in_specs=in_specs, out_specs=out_specs, check_vma=False)
```
